32 devices in a mesh: sp: 8 (over z, x), dp: 4 (over y, core).
Axes of the slice: x: 2, y: 2, z: 4, core: 2. Of those that a mesh axis runs over, the one named last changes fastest.
Arguments:
- activations: bfloat16 [4, 4096, 2048], P('dp', 'sp'), may hold values from -6 to 6
- value_weight: bfloat16 [2048, 1024], P(('sp', 'dp')), may hold values from -0.125 to 0.125
- gate_weight: bfloat16 [2048, 1024], P(('sp', 'dp')), may hold values from -0.125 to 0.125
- input_weight: bfloat16 [2048, 512], P(('sp', 'dp')), may hold values from -0.125 to 0.125
- readout_weight: bfloat16 [2048, 512], P(('sp', 'dp')), may hold values from -0.125 to 0.125
- rate_weight: bfloat16 [2048, 16], replicated, may hold values from -0.125 to 0.125
- value_taps: bfloat16 [4, 1024], replicated, may hold values from -0.375 to 0.375
- input_taps: bfloat16 [4, 512], replicated, may hold values from -3 to 3
- readout_taps: bfloat16 [4, 512], replicated, may hold values from -3 to 3
- rate_bias: float32 [16], replicated, may hold values from -1 to 1
- decay_log: float32 [16], replicated, may hold values from -1 to 1.5
- norm_gain: float32 [1024], replicated, may hold values from 0.1 to 1.9
- out_weight: bfloat16 [1024, 2048], P(None, ('sp', 'dp')), may hold values from -0.1875 to 0.1875
Outputs:
- mixed_out: bfloat16 [4, 4096, 2048], P('dp', 'sp')
The draws below stay inside these ranges and needn't reach their ends.
All inputs are finite; a program needn't handle non-finite values.
Results may differ from the reference program's by a relative error of at most 0.014.
Values may be sent and summed in bfloat16 or wider, within the bound.
No kernel may reach another device: no remote copies, remote signals or barrier semaphores. Data moves between devices by JAX's collectives and lax.ppermute only.
A program may use at most 128 MiB of HBM per device.

```python
import jax
import jax.numpy as jnp
from jax import lax

D = 2048
HEADS = 16
HEAD_DIM = 64
GROUPS = 4
STATE = 128
CONV = 4
BLOCK = 64
WIDTH = 1024
LENGTH = 4096
SEQS = 4


def shard_levels(key, dims, shards, least, high):
    factor_of = 1.0
    for dim, blocks in shards:
        steps = jax.random.uniform(jax.random.fold_in(jax.random.fold_in(key, 6), dim), (blocks,), jnp.float32, least / len(shards), high / len(shards))
        factor_of = factor_of * jnp.repeat(jnp.exp(steps), dims[dim] // blocks).reshape((-1,) + (1,) * (len(dims) - 1 - dim))
    return factor_of


def normal_values(rng, shape, scale, reach, shards=(), kind=jnp.bfloat16):
    level = shard_levels(rng, shape, shards, -0.22, 0.18) if shards else 1.0
    entries = jax.random.normal(rng, shape, jnp.float32) * scale * level
    return jnp.minimum(jnp.maximum(entries, -reach), reach).astype(kind)


def setup_inputs(seed: int = 0) -> dict:
    streams_of = jax.random.split(jax.random.key(seed), 14)
    return {
        "activations": normal_values(streams_of[0], (SEQS, LENGTH, D), 1.0, 6.0, ((0, 4), (1, 8))),
        "value_weight": normal_values(streams_of[1], (D, WIDTH), D ** -0.5, 0.125, ((0, 32),)),
        "gate_weight": normal_values(streams_of[2], (D, WIDTH), D ** -0.5, 0.125, ((0, 32),)),
        "input_weight": normal_values(streams_of[3], (D, GROUPS * STATE), D ** -0.5, 0.125, ((0, 32),)),
        "readout_weight": normal_values(streams_of[4], (D, GROUPS * STATE), D ** -0.5, 0.125, ((0, 32),)),
        "rate_weight": normal_values(streams_of[5], (D, HEADS), D ** -0.5, 0.125),
        "value_taps": normal_values(streams_of[6], (CONV, WIDTH), (64 * CONV) ** -0.5, 0.375),
        "input_taps": normal_values(streams_of[7], (CONV, GROUPS * STATE), CONV ** -0.5, 3.0),
        "readout_taps": normal_values(streams_of[8], (CONV, GROUPS * STATE), CONV ** -0.5, 3.0),
        "rate_bias": jnp.clip(jax.random.uniform(streams_of[9], (HEADS,), jnp.float32, -1.0, 1.0), -1.0, 1.0),
        "decay_log": jnp.clip(jax.random.uniform(streams_of[10], (HEADS,), jnp.float32, -1.0, 1.5), -1.0, 1.5),
        "norm_gain": jnp.clip(1.0 + 0.18 * jax.random.normal(streams_of[11], (WIDTH,), jnp.float32), 0.1, 1.9),
        "out_weight": normal_values(streams_of[12], (WIDTH, D), WIDTH ** -0.5, 0.1875, ((1, 32),)),
    }


norm_eps = 1.0

def broaden(matrix, groups, head_count):
    row_count = matrix.shape[0]
    group_width = matrix.shape[1] // groups
    spread = matrix.reshape(row_count, groups, 1, group_width)
    spread = jnp.broadcast_to(spread, (row_count, groups, head_count // groups, group_width))
    return spread.reshape(row_count, head_count * group_width)

def causal_conv(series, kernel):
    extent = kernel.shape[0]
    length = series.shape[0]
    padded = jnp.pad(series.astype(jnp.float32), ((extent - 1, 0), (0, 0)))
    result = jnp.zeros(series.shape, jnp.float32)
    for offset in range(extent):
        result = result + kernel[offset].astype(jnp.float32) * padded[offset:offset + length]
    return result

def state_mix(values, inputs, readouts, rates, decay):
    length, head_count, head_width = values.shape
    blocks = length // BLOCK
    block_values = values.reshape(blocks, BLOCK, head_count, head_width).astype(jnp.float32)
    block_inputs = inputs.reshape(blocks, BLOCK, head_count, -1).astype(jnp.float32)
    block_reads = readouts.reshape(blocks, BLOCK, head_count, -1).astype(jnp.float32)
    block_rates = rates.reshape(blocks, BLOCK, head_count)
    running = jnp.cumsum(block_rates * decay, axis=1)
    by_head = jnp.transpose(running, (0, 2, 1))
    rate_head = jnp.transpose(block_rates, (0, 2, 1))
    causal = jnp.tril(jnp.ones((BLOCK, BLOCK), dtype=bool))
    intervals = by_head[:, :, :, None] - by_head[:, :, None, :]
    fading = jnp.where(causal, jnp.exp(jnp.minimum(intervals, 0.0)), 0.0)
    intersect = jnp.einsum('bthn,bshn->bhts', block_reads, block_inputs)
    scores = (intersect * fading * rate_head[:, :, None, :]).astype(jnp.bfloat16)
    within = jnp.einsum('bhts,bshp->bthp', scores.astype(jnp.float32), block_values)
    tail_fade = jnp.exp(running[:, -1:, :] - running) * block_rates
    weighted = (block_values * tail_fade[:, :, :, None]).astype(jnp.bfloat16)
    states = jnp.einsum('bshp,bshn->bhpn', weighted.astype(jnp.float32), block_inputs)
    totals = jnp.cumsum(running[:, -1, :], axis=0)
    starts = totals - running[:, -1, :]
    earlier = jnp.tril(jnp.ones((blocks, blocks), dtype=bool), -1)
    carried = jnp.where(earlier[:, :, None], jnp.exp(jnp.minimum(starts[:, None, :] - totals[None, :, :], 0.0)), 0.0)
    entering = jnp.einsum('cdh,dhpn->chpn', carried, states, precision=lax.Precision.HIGHEST)
    across = jnp.einsum('bthn,bhpn->bthp', block_reads, entering, precision=lax.Precision.HIGHEST)
    across = across * jnp.exp(running)[:, :, :, None]
    return (within + across).reshape(length, head_count * head_width)

def reference(activations, value_weight, gate_weight, input_weight, readout_weight, rate_weight, value_taps, input_taps, readout_taps, rate_bias, decay_log, norm_gain, out_weight):

    def mixer(sequence):
        length = sequence.shape[0]
        projected = jnp.dot(sequence, value_weight, preferred_element_type=jnp.float32).astype(jnp.bfloat16)
        gate_proj = jnp.dot(sequence, gate_weight, preferred_element_type=jnp.float32).astype(jnp.bfloat16)
        input_proj = jnp.dot(sequence, input_weight, preferred_element_type=jnp.float32).astype(jnp.bfloat16)
        readout_proj = jnp.dot(sequence, readout_weight, preferred_element_type=jnp.float32).astype(jnp.bfloat16)
        rate_raw = jnp.dot(sequence, rate_weight, preferred_element_type=jnp.float32).astype(jnp.bfloat16)
        conv_values = jax.nn.silu(causal_conv(projected, value_taps)).astype(jnp.bfloat16)
        conv_inputs = jax.nn.silu(causal_conv(input_proj, input_taps)).astype(jnp.bfloat16)
        conv_reads = jax.nn.silu(causal_conv(readout_proj, readout_taps)).astype(jnp.bfloat16)
        head_inputs = broaden(conv_inputs, GROUPS, HEADS).reshape(length, HEADS, STATE)
        head_reads = broaden(conv_reads, GROUPS, HEADS).reshape(length, HEADS, STATE)
        rates = jax.nn.softplus(rate_raw.astype(jnp.float32) + rate_bias)
        decay = -jnp.exp(decay_log) / length
        mixed = state_mix(conv_values.reshape(length, HEADS, HEAD_DIM), head_inputs, head_reads, rates, decay).astype(jnp.bfloat16)
        gated = mixed.astype(jnp.float32) * jax.nn.silu(gate_proj.astype(jnp.float32))
        scale = lax.rsqrt(lax.optimization_barrier(jnp.mean(gated * gated, axis=-1, keepdims=True)) + norm_eps)
        normed = (gated * scale * norm_gain).astype(jnp.bfloat16)
        return jnp.dot(normed, out_weight, preferred_element_type=jnp.float32).astype(jnp.bfloat16)
    return lax.map(mixer, activations)
```

```python
import functools

import jax
import jax.numpy as jnp
from jax import lax
from jax.experimental import pallas as pl
from jax.experimental.pallas import tpu as pltpu
from jax.sharding import PartitionSpec as P

GROUPS = 4
CHUNK = 128
HALO = 16
norm_eps = 1.0
F32 = jnp.float32
BF16 = jnp.bfloat16


def conv_silu(ref, start, taps_ref, col, width):
    x = ref[pl.ds(start, CHUNK + HALO), col : col + width].astype(F32)
    extent = taps_ref.shape[0]
    total = None
    for k in range(extent):
        shift = extent - 1 - k
        moved = pltpu.roll(x, shift, 0) if shift else x
        term = taps_ref[k : k + 1, col : col + width].astype(F32) * moved[HALO:]
        total = term if total is None else total + term
    return (total / (1.0 + jnp.exp(-total))).astype(BF16)


def states_kernel(
    v_ref, b_ref, vt_ref, bt_ref, tail_ref, cdec_ref, cv_ref, cb_ref, cr_ref, prefix_ref, final_ref
):
    c = pl.program_id(0)
    start = c * CHUNK
    state = cb_ref.shape[1] // GROUPS
    wide = cv_ref.shape[1] // GROUPS

    @pl.when(c == 0)
    def _():
        final_ref[...] = jnp.zeros(final_ref.shape, F32)

    for g in range(GROUPS):
        values = conv_silu(v_ref, start, vt_ref, g * wide, wide)
        cv_ref[:, g * wide : (g + 1) * wide] = values
        inputs = conv_silu(b_ref, start, bt_ref, g * state, state)
        cb_ref[:, g * state : (g + 1) * state] = inputs
        reads = conv_silu(b_ref, start, bt_ref, (GROUPS + g) * state, state)
        cr_ref[:, g * state : (g + 1) * state] = reads
        weighted = (values.astype(F32) * tail_ref[:, g * wide : (g + 1) * wide]).astype(BF16)
        added = lax.dot_general(inputs, weighted, (((0,), (0,)), ((), ())), preferred_element_type=F32)
        rows = slice(g * state, (g + 1) * state)
        old = final_ref[rows, :]
        prefix_ref[0, rows, :] = old.astype(BF16)
        keep = cdec_ref[pl.ds(c, 1), g * wide : (g + 1) * wide]
        final_ref[rows, :] = old * keep + added


def within_kernel(cv_ref, cb_ref, cr_ref, prefix_ref, cum_ref, cumt_ref, ratet_ref, erun_ref, out_ref):
    state = cb_ref.shape[1] // GROUPS
    wide = cv_ref.shape[1] // GROUPS
    heads = cum_ref.shape[1]
    width = cv_ref.shape[1] // heads
    per_group = heads // GROUPS
    t = lax.broadcasted_iota(jnp.int32, (CHUNK, CHUNK), 0)
    s = lax.broadcasted_iota(jnp.int32, (CHUNK, CHUNK), 1)
    causal = s <= t
    low = lax.broadcasted_iota(jnp.int32, (CHUNK, 2 * width), 1) < width
    zero = jnp.zeros((CHUNK, 2 * width), BF16)
    for g in range(GROUPS):
        reads = cr_ref[:, g * state : (g + 1) * state]
        inputs = cb_ref[:, g * state : (g + 1) * state]
        inter = lax.dot_general(reads, inputs, (((1,), (1,)), ((), ())), preferred_element_type=F32)
        across = jnp.dot(reads, prefix_ref[0, g * state : (g + 1) * state, :], preferred_element_type=F32)
        for pair in range(per_group // 2):
            scores = []
            for j in range(2):
                h = g * per_group + 2 * pair + j
                gap = jnp.minimum(cum_ref[:, h : h + 1] - cumt_ref[h : h + 1, :], 0.0)
                sc = inter * jnp.exp(gap) * ratet_ref[h : h + 1, :]
                scores.append(jnp.where(causal, sc, 0.0).astype(BF16))
            col = g * wide + pair * 2 * width
            vals = cv_ref[:, col : col + 2 * width]
            split = jnp.concatenate([jnp.where(low, vals, zero), jnp.where(low, zero, vals)], axis=0)
            inside = jnp.dot(jnp.concatenate(scores, axis=1), split, preferred_element_type=F32)
            part = across[:, pair * 2 * width : (pair + 1) * 2 * width]
            out_ref[:, col : col + 2 * width] = inside + part * erun_ref[:, col : col + 2 * width]


def finish_kernel(part_ref, cr_ref, enter_ref, ecum_ref, *rest):
    gate_refs, (gain_ref, out_ref) = rest[:-2], rest[-2:]
    state = cr_ref.shape[1] // GROUPS
    wide = part_ref.shape[1] // GROUPS
    pieces = []
    for g in range(GROUPS):
        reads = cr_ref[:, g * state : (g + 1) * state]
        far = jnp.dot(reads, enter_ref[g * state : (g + 1) * state, :], preferred_element_type=F32)
        cols = slice(g * wide, (g + 1) * wide)
        pieces.append((part_ref[:, cols] + far * ecum_ref[:, cols]).astype(BF16).astype(F32))
    mixed = jnp.concatenate(pieces, axis=1)
    gate = jnp.concatenate([r[...] for r in gate_refs], axis=1).astype(F32)
    gated = mixed * (gate / (1.0 + jnp.exp(-gate)))
    scale = lax.rsqrt(jnp.mean(gated * gated, axis=-1, keepdims=True) + norm_eps)
    out_ref[...] = (gated * scale * gain_ref[...]).astype(BF16)


def whole(shape):
    return pl.BlockSpec(shape, lambda c: (0,) * len(shape))


def rows(width):
    return pl.BlockSpec((CHUNK, width), lambda c: (c, 0))


def shift_before(x, axis, size, distance):
    return lax.ppermute(x, axis, [(i, i + distance) for i in range(size - distance)])


def sequence_part(values, mix, gates, taps, rate_raw, rate_bias, decay_log, norm_gain, length, sp, index):
    value_taps, mix_taps = taps
    local = values.shape[0] - HALO
    chunks = local // CHUNK
    width = values.shape[1]
    heads = rate_bias.shape[0]
    wide = width // GROUPS
    keys = mix.shape[1] // 2
    state = keys // GROUPS
    spread = functools.partial(jnp.repeat, repeats=width // heads, axis=1)
    rate = jax.nn.softplus(rate_raw.astype(F32) + rate_bias)
    decay = -jnp.exp(decay_log) / length
    tri = jnp.tril(jnp.ones((local, local), F32))
    cum = jnp.dot(tri, rate * decay, precision=lax.Precision.HIGHEST)
    ends = cum[CHUNK - 1 :: CHUNK]
    starts = jnp.concatenate([jnp.zeros((1, heads), F32), ends[:-1]], axis=0)
    end_rows = jnp.repeat(ends, CHUNK, axis=0)
    start_rows = jnp.repeat(starts, CHUNK, axis=0)
    tail = spread(jnp.exp(jnp.minimum(end_rows - cum, 0.0)) * rate)
    erun = spread(jnp.exp(jnp.minimum(cum - start_rows, 0.0)))
    ecum = spread(jnp.exp(cum))
    cdec = spread(jnp.exp(ends - starts))
    cumt = cum.T
    ratet = rate.T
    totals = lax.all_gather(cum[-1], "sp")
    tail, erun, ecum, cdec, cumt, ratet, totals = lax.optimization_barrier(
        (tail, erun, ecum, cdec, cumt, ratet, totals)
    )
    arb = pltpu.CompilerParams(dimension_semantics=("arbitrary",))
    cv, cb, cr, prefix, final = pl.pallas_call(
        states_kernel,
        grid=(chunks,),
        in_specs=[
            whole(values.shape),
            whole(mix.shape),
            whole(value_taps.shape),
            whole(mix_taps.shape),
            rows(width),
            whole(cdec.shape),
        ],
        out_specs=[
            rows(width),
            rows(keys),
            rows(keys),
            pl.BlockSpec((1, keys, wide), lambda c: (c, 0, 0)),
            whole((keys, wide)),
        ],
        out_shape=[
            jax.ShapeDtypeStruct((local, width), BF16),
            jax.ShapeDtypeStruct((local, keys), BF16),
            jax.ShapeDtypeStruct((local, keys), BF16),
            jax.ShapeDtypeStruct((chunks, keys, wide), BF16),
            jax.ShapeDtypeStruct((keys, wide), F32),
        ],
        compiler_params=arb,
        name="states",
    )(values, mix, value_taps, mix_taps, tail, cdec)
    device = lax.broadcasted_iota(jnp.int32, (sp, 1), 0)
    own = spread(jnp.exp(cum[-1:]))

    def by_head(row):
        return jnp.repeat(row.reshape(GROUPS, 1, wide), state, axis=1).reshape(keys, wide)

    own = by_head(own)
    entering = None
    window = 0
    while window < sp - 1:
        inclusive = final if entering is None else final + own * entering
        got = shift_before(inclusive.astype(BF16), "sp", sp, window + 1).astype(F32)
        if entering is None:
            entering = got
        else:
            near = (device >= index - window) & (device < index)
            span = jnp.sum(jnp.where(near, totals, 0.0), axis=0, keepdims=True)
            entering = entering + by_head(spread(jnp.exp(span))) * got
        window = 2 * window + 1
    entering = entering.astype(BF16) if entering is not None else jnp.zeros((keys, wide), BF16)
    part = pl.pallas_call(
        within_kernel,
        grid=(chunks,),
        in_specs=[
            rows(width),
            rows(keys),
            rows(keys),
            pl.BlockSpec((1, keys, wide), lambda c: (c, 0, 0)),
            rows(heads),
            pl.BlockSpec((heads, CHUNK), lambda c: (0, c)),
            pl.BlockSpec((heads, CHUNK), lambda c: (0, c)),
            rows(width),
        ],
        out_specs=rows(width),
        out_shape=jax.ShapeDtypeStruct((local, width), F32),
        compiler_params=arb,
        name="within",
    )(cv, cb, cr, prefix, cum, cumt, ratet, erun)
    return pl.pallas_call(
        finish_kernel,
        grid=(chunks,),
        in_specs=[rows(width), rows(keys), whole((keys, wide)), rows(width)]
        + [rows(g.shape[1]) for g in gates]
        + [whole((1, width))],
        out_specs=rows(width),
        out_shape=jax.ShapeDtypeStruct((local, width), BF16),
        compiler_params=arb,
        name="finish",
    )(part, cr, entering, ecum, *gates, norm_gain.reshape(1, width))


def make_per_device(mesh):
    sp = mesh.shape["sp"]

    def per_device(
        activations,
        value_weight,
        gate_weight,
        input_weight,
        readout_weight,
        rate_weight,
        value_taps,
        input_taps,
        readout_taps,
        rate_bias,
        decay_log,
        norm_gain,
        out_weight,
    ):
        own = activations[0]
        index = lax.axis_index("sp")
        halo = shift_before(own[-HALO:], "sp", sp, 1)
        joined = jnp.concatenate([value_weight, input_weight, readout_weight, gate_weight], axis=1)
        weights = lax.all_gather(joined, ("sp", "dp"), axis=0, tiled=True)
        out_rows = lax.all_gather(out_weight.T, ("sp", "dp"), axis=0, tiled=True)
        sequence = jnp.concatenate([halo, own], axis=0)
        rate_raw = jnp.dot(own, rate_weight, preferred_element_type=F32).astype(BF16)
        width = value_weight.shape[1]
        keys = input_weight.shape[1]
        values = jnp.dot(sequence, weights[:, :width], preferred_element_type=F32).astype(BF16)
        mix = jnp.dot(
            sequence, weights[:, width : width + 2 * keys], preferred_element_type=F32
        ).astype(BF16)
        gate = jnp.dot(own, weights[:, width + 2 * keys :], preferred_element_type=F32).astype(BF16)
        taps = (value_taps, jnp.concatenate([input_taps, readout_taps], axis=1))
        normed = sequence_part(
            values, mix, (gate,), taps, rate_raw, rate_bias, decay_log, norm_gain,
            own.shape[0] * sp, sp, index,
        )
        result = lax.dot_general(
            normed, out_rows, (((1,), (1,)), ((), ())), preferred_element_type=F32
        )
        return result.astype(BF16)[None]

    return per_device


def solution(mesh):
    rows_split = P(("sp", "dp"), None)
    placed = (P("dp", "sp", None),) + (rows_split,) * 4 + (P(),) * 7 + (P(None, ("sp", "dp")),)
    return jax.shard_map(
        make_per_device(mesh),
        mesh=mesh,
        in_specs=placed,
        out_specs=P("dp", "sp", None),
        check_vma=False,
    )
```

```python
import functools

import jax
import jax.numpy as jnp
from jax import lax
from jax.experimental import pallas as pl
from jax.experimental.pallas import tpu as pltpu
from jax.sharding import PartitionSpec as P

GROUPS = 4
CHUNK = 128
HALO = 16
norm_eps = 1.0
F32 = jnp.float32
BF16 = jnp.bfloat16


def conv_silu(ref, start, taps_ref, col, width):
    x = ref[pl.ds(start, CHUNK + HALO), col : col + width].astype(F32)
    extent = taps_ref.shape[0]
    total = None
    for k in range(extent):
        shift = extent - 1 - k
        moved = pltpu.roll(x, shift, 0) if shift else x
        term = taps_ref[k : k + 1, col : col + width].astype(F32) * moved[HALO:]
        total = term if total is None else total + term
    return (total / (1.0 + jnp.exp(-total))).astype(BF16)


def states_kernel(
    v_ref, b_ref, vt_ref, bt_ref, tail_ref, cdec_ref, cv_ref, cb_ref, cr_ref, prefix_ref, final_ref
):
    c = pl.program_id(0)
    start = c * CHUNK
    state = cb_ref.shape[1] // GROUPS
    wide = cv_ref.shape[1] // GROUPS

    @pl.when(c == 0)
    def _():
        final_ref[...] = jnp.zeros(final_ref.shape, F32)

    for g in range(GROUPS):
        values = conv_silu(v_ref, start, vt_ref, g * wide, wide)
        cv_ref[:, g * wide : (g + 1) * wide] = values
        inputs = conv_silu(b_ref, start, bt_ref, g * state, state)
        cb_ref[:, g * state : (g + 1) * state] = inputs
        reads = conv_silu(b_ref, start, bt_ref, (GROUPS + g) * state, state)
        cr_ref[:, g * state : (g + 1) * state] = reads
        weighted = (values.astype(F32) * tail_ref[:, g * wide : (g + 1) * wide]).astype(BF16)
        added = lax.dot_general(inputs, weighted, (((0,), (0,)), ((), ())), preferred_element_type=F32)
        rows = slice(g * state, (g + 1) * state)
        old = final_ref[rows, :]
        prefix_ref[0, rows, :] = old.astype(BF16)
        keep = cdec_ref[pl.ds(c, 1), g * wide : (g + 1) * wide]
        final_ref[rows, :] = old * keep + added


def within_kernel(cv_ref, cb_ref, cr_ref, prefix_ref, cum_ref, cumt_ref, ratet_ref, erun_ref, out_ref):
    state = cb_ref.shape[1] // GROUPS
    wide = cv_ref.shape[1] // GROUPS
    heads = cum_ref.shape[1]
    width = cv_ref.shape[1] // heads
    per_group = heads // GROUPS
    t = lax.broadcasted_iota(jnp.int32, (CHUNK, CHUNK), 0)
    s = lax.broadcasted_iota(jnp.int32, (CHUNK, CHUNK), 1)
    causal = s <= t
    low = lax.broadcasted_iota(jnp.int32, (CHUNK, 2 * width), 1) < width
    zero = jnp.zeros((CHUNK, 2 * width), BF16)
    for g in range(GROUPS):
        reads = cr_ref[:, g * state : (g + 1) * state]
        inputs = cb_ref[:, g * state : (g + 1) * state]
        inter = lax.dot_general(reads, inputs, (((1,), (1,)), ((), ())), preferred_element_type=F32)
        across = jnp.dot(reads, prefix_ref[0, g * state : (g + 1) * state, :], preferred_element_type=F32)
        for pair in range(per_group // 2):
            scores = []
            for j in range(2):
                h = g * per_group + 2 * pair + j
                gap = jnp.minimum(cum_ref[:, h : h + 1] - cumt_ref[h : h + 1, :], 0.0)
                sc = inter * jnp.exp(gap) * ratet_ref[h : h + 1, :]
                scores.append(jnp.where(causal, sc, 0.0).astype(BF16))
            col = g * wide + pair * 2 * width
            vals = cv_ref[:, col : col + 2 * width]
            split = jnp.concatenate([jnp.where(low, vals, zero), jnp.where(low, zero, vals)], axis=0)
            inside = jnp.dot(jnp.concatenate(scores, axis=1), split, preferred_element_type=F32)
            part = across[:, pair * 2 * width : (pair + 1) * 2 * width]
            out_ref[:, col : col + 2 * width] = inside + part * erun_ref[:, col : col + 2 * width]


def finish_kernel(part_ref, cr_ref, enter_ref, ecum_ref, *rest):
    gate_refs, (gain_ref, out_ref) = rest[:-2], rest[-2:]
    state = cr_ref.shape[1] // GROUPS
    wide = part_ref.shape[1] // GROUPS
    pieces = []
    for g in range(GROUPS):
        reads = cr_ref[:, g * state : (g + 1) * state]
        far = jnp.dot(reads, enter_ref[g * state : (g + 1) * state, :], preferred_element_type=F32)
        cols = slice(g * wide, (g + 1) * wide)
        pieces.append((part_ref[:, cols] + far * ecum_ref[:, cols]).astype(BF16).astype(F32))
    mixed = jnp.concatenate(pieces, axis=1)
    gate = jnp.concatenate([r[...] for r in gate_refs], axis=1).astype(F32)
    gated = mixed * (gate / (1.0 + jnp.exp(-gate)))
    scale = lax.rsqrt(jnp.mean(gated * gated, axis=-1, keepdims=True) + norm_eps)
    out_ref[...] = (gated * scale * gain_ref[...]).astype(BF16)


def whole(shape):
    return pl.BlockSpec(shape, lambda c: (0,) * len(shape))


def rows(width):
    return pl.BlockSpec((CHUNK, width), lambda c: (c, 0))


def shift_before(x, axis, size, distance):
    return lax.ppermute(x, axis, [(i, i + distance) for i in range(size - distance)])


def sequence_part(values, mix, gates, taps, rate_raw, rate_bias, decay_log, norm_gain, length, sp, index):
    value_taps, mix_taps = taps
    local = values.shape[0] - HALO
    chunks = local // CHUNK
    width = values.shape[1]
    heads = rate_bias.shape[0]
    wide = width // GROUPS
    keys = mix.shape[1] // 2
    state = keys // GROUPS
    spread = functools.partial(jnp.repeat, repeats=width // heads, axis=1)
    rate = jax.nn.softplus(rate_raw.astype(F32) + rate_bias)
    decay = -jnp.exp(decay_log) / length
    tri = jnp.tril(jnp.ones((local, local), F32))
    cum = jnp.dot(tri, rate * decay, precision=lax.Precision.HIGHEST)
    ends = cum[CHUNK - 1 :: CHUNK]
    starts = jnp.concatenate([jnp.zeros((1, heads), F32), ends[:-1]], axis=0)
    end_rows = jnp.repeat(ends, CHUNK, axis=0)
    start_rows = jnp.repeat(starts, CHUNK, axis=0)
    tail = spread(jnp.exp(jnp.minimum(end_rows - cum, 0.0)) * rate)
    erun = spread(jnp.exp(jnp.minimum(cum - start_rows, 0.0)))
    ecum = spread(jnp.exp(cum))
    cdec = spread(jnp.exp(ends - starts))
    cumt = cum.T
    ratet = rate.T
    totals = lax.all_gather(cum[-1], "sp")
    tail, erun, ecum, cdec, cumt, ratet, totals = lax.optimization_barrier(
        (tail, erun, ecum, cdec, cumt, ratet, totals)
    )
    arb = pltpu.CompilerParams(dimension_semantics=("arbitrary",))
    cv, cb, cr, prefix, final = pl.pallas_call(
        states_kernel,
        grid=(chunks,),
        in_specs=[
            whole(values.shape),
            whole(mix.shape),
            whole(value_taps.shape),
            whole(mix_taps.shape),
            rows(width),
            whole(cdec.shape),
        ],
        out_specs=[
            rows(width),
            rows(keys),
            rows(keys),
            pl.BlockSpec((1, keys, wide), lambda c: (c, 0, 0)),
            whole((keys, wide)),
        ],
        out_shape=[
            jax.ShapeDtypeStruct((local, width), BF16),
            jax.ShapeDtypeStruct((local, keys), BF16),
            jax.ShapeDtypeStruct((local, keys), BF16),
            jax.ShapeDtypeStruct((chunks, keys, wide), BF16),
            jax.ShapeDtypeStruct((keys, wide), F32),
        ],
        compiler_params=arb,
        name="states",
    )(values, mix, value_taps, mix_taps, tail, cdec)
    device = lax.broadcasted_iota(jnp.int32, (sp, 1), 0)
    own = spread(jnp.exp(cum[-1:]))

    def by_head(row):
        return jnp.repeat(row.reshape(GROUPS, 1, wide), state, axis=1).reshape(keys, wide)

    own = by_head(own)
    entering = None
    window = 0
    while window < sp - 1:
        inclusive = final if entering is None else final + own * entering
        got = shift_before(inclusive.astype(BF16), "sp", sp, window + 1).astype(F32)
        if entering is None:
            entering = got
        else:
            near = (device >= index - window) & (device < index)
            span = jnp.sum(jnp.where(near, totals, 0.0), axis=0, keepdims=True)
            entering = entering + by_head(spread(jnp.exp(span))) * got
        window = 2 * window + 1
    entering = entering.astype(BF16) if entering is not None else jnp.zeros((keys, wide), BF16)
    part = pl.pallas_call(
        within_kernel,
        grid=(chunks,),
        in_specs=[
            rows(width),
            rows(keys),
            rows(keys),
            pl.BlockSpec((1, keys, wide), lambda c: (c, 0, 0)),
            rows(heads),
            pl.BlockSpec((heads, CHUNK), lambda c: (0, c)),
            pl.BlockSpec((heads, CHUNK), lambda c: (0, c)),
            rows(width),
        ],
        out_specs=rows(width),
        out_shape=jax.ShapeDtypeStruct((local, width), F32),
        compiler_params=arb,
        cost_estimate=pl.CostEstimate(
            flops=8 * local * width * (CHUNK + state), transcendentals=0, bytes_accessed=9 * local * width
        ),
        name="within",
    )(cv, cb, cr, prefix, cum, cumt, ratet, erun)
    return pl.pallas_call(
        finish_kernel,
        grid=(chunks,),
        in_specs=[rows(width), rows(keys), whole((keys, wide)), rows(width)]
        + [rows(g.shape[1]) for g in gates]
        + [whole((1, width))],
        out_specs=rows(width),
        out_shape=jax.ShapeDtypeStruct((local, width), BF16),
        compiler_params=arb,
        name="finish",
    )(part, cr, entering, ecum, *gates, norm_gain.reshape(1, width))


def axis_sizes(mesh):
    sp, dp = mesh.shape["sp"], mesh.shape["dp"]
    x = 1
    while sp % (4 * x * x) == 0:
        x *= 2
    core = 2 if dp % 2 == 0 else 1
    return (sp // x, x, dp // core, core)


def shifted(x, sizes, axis, distance):
    total = sizes[0] * sizes[1] * sizes[2] * sizes[3]
    stride = 1
    for later in sizes[axis + 1 :]:
        stride *= later
    pairs = []
    for i in range(total):
        place = (i // stride) % sizes[axis]
        pairs.append((i, i + ((place + distance) % sizes[axis] - place) * stride))
    return lax.ppermute(x, ("sp", "dp"), pairs)


def gather_pieces(block, sizes, order):
    line = [block] + [shifted(block, sizes, 0, k) for k in range(1, sizes[0])]
    pieces = {(0, 0, 0): jnp.concatenate(line, axis=0)}
    for axis in order:
        for place, piece in list(pieces.items()):
            for k in range(1, sizes[axis]):
                there = list(place)
                there[3 - axis] = k
                pieces[tuple(there)] = shifted(piece, sizes, axis, k)
    return pieces


def project(sequence, pieces, sizes):
    total = None
    depth = next(iter(pieces.values())).shape[0]
    for place, piece in pieces.items():
        at = (place[0] * sizes[2] + place[1]) * sizes[1] + place[2]
        part = jnp.dot(
            sequence[:, at * depth : (at + 1) * depth], piece, preferred_element_type=F32
        )
        total = part if total is None else total + part
    return total.astype(BF16)


def relative_columns(sequence, sizes, sp_index, dp_index, block):
    z, x, y, core = sizes
    here = (sp_index // x, sp_index % x, dp_index // core, dp_index % core)
    depth = sequence.shape[1]
    j = lax.broadcasted_iota(jnp.int32, (1, depth), 1)
    row = j % block
    piece = j // block
    back = (piece % z, (piece // z) % x, (piece // (z * x)) % y, piece // (z * x * y))
    at = [(h - b + n) % n for h, b, n in zip(here, back, sizes)]
    source = (((at[0] * x + at[1]) * y + at[2]) * core + at[3]) * block + row
    select = (lax.broadcasted_iota(jnp.int32, (depth, 1), 0) == source).astype(BF16)
    return jnp.dot(sequence, select, preferred_element_type=F32).astype(BF16)


def make_per_device(mesh):
    sp = mesh.shape["sp"]
    sizes = axis_sizes(mesh)

    def per_device(
        activations,
        value_weight,
        gate_weight,
        input_weight,
        readout_weight,
        rate_weight,
        value_taps,
        input_taps,
        readout_taps,
        rate_bias,
        decay_log,
        norm_gain,
        out_weight,
    ):
        own = activations[0]
        index = lax.axis_index("sp")
        halo = shift_before(own[-HALO:], "sp", sp, 1)
        joined = jnp.concatenate([value_weight, input_weight, readout_weight], axis=1)
        weights = lax.all_gather(joined, ("sp", "dp"), axis=0, tiled=True)
        out_rows = lax.all_gather(out_weight.T, ("sp", "dp"), axis=0, tiled=True)
        rate_raw = jnp.dot(own, rate_weight, preferred_element_type=F32).astype(BF16)
        sequence = jnp.concatenate([halo, own], axis=0)
        turned = relative_columns(
            own, sizes, index, lax.axis_index("dp"), value_weight.shape[0]
        )
        gates = (project(turned, gather_pieces(gate_weight, sizes, (1, 2, 3)), sizes),)
        width = value_weight.shape[1]
        values = jnp.dot(sequence, weights[:, :width], preferred_element_type=F32).astype(BF16)
        mix = jnp.dot(sequence, weights[:, width:], preferred_element_type=F32).astype(BF16)
        taps = (value_taps, jnp.concatenate([input_taps, readout_taps], axis=1))
        normed = sequence_part(
            values, mix, gates, taps, rate_raw, rate_bias, decay_log, norm_gain,
            own.shape[0] * sp, sp, index,
        )
        result = lax.dot_general(
            normed, out_rows, (((1,), (1,)), ((), ())), preferred_element_type=F32
        )
        return result.astype(BF16)[None]

    return per_device


def solution(mesh):
    rows_split = P(("sp", "dp"), None)
    placed = (P("dp", "sp", None),) + (rows_split,) * 4 + (P(),) * 7 + (P(None, ("sp", "dp")),)
    return jax.shard_map(
        make_per_device(mesh),
        mesh=mesh,
        in_specs=placed,
        out_specs=P("dp", "sp", None),
        check_vma=False,
    )
```
